32 devices in a mesh: ep: 8 (over z, x), tp: 4 (over y, core).
Axes of the slice: x: 2, y: 2, z: 4, core: 2. Of those that a mesh axis runs over, the one named last changes fastest.
Arguments:
- tokens: bfloat16 [4096, 4096], P('ep', 'tp'), may hold values from -100 to 100, as said below
- routes: int32 [4096, 2], P('ep'), may hold values from 0 to 15, all different within a row; in each aligned block of 512 rows (0 to 511, 512 to 1023, ...) at most 128 rows name the same one
- route_weights: float32 [4096, 2], P('ep'), may hold values from 0.1 to 1
- norm_gain: float32 [4096], P('tp'), may hold values from 0.1 to 1.9
- gate_weight: bfloat16 [16, 4096, 512], P('ep', 'tp'), may hold values from -0.09375 to 0.09375
- up_weight: bfloat16 [16, 4096, 512], P('ep', 'tp'), may hold values from -0.09375 to 0.09375
- down_weight: bfloat16 [16, 512, 4096], P('ep', None, 'tp'), may hold values from -0.25 to 0.25
- final_gain: float32 [4096], P('tp'), may hold values from 0.1 to 1.9
Outputs:
- mixed: bfloat16 [4096, 4096], P('ep', 'tp')
The draws below stay inside these ranges and needn't reach their ends.
Inputs may be any that keep to these rules, and one draw needn't show every extreme that they name: `tokens`: real-valued activations whose features differ in scale. `routes`: each row names 2 different experts; among the 512 rows of one aligned block no expert is named more than 128 times, a bound that some block reaches.
All inputs are finite; a program needn't handle non-finite values.
Results may differ from the reference program's by a relative error of at most 0.018.
Values may be sent and summed in bfloat16 or wider, within the bound.
A program may use at most 64 MiB of HBM per device.

```python
import math
import jax
import jax.numpy as jnp
import numpy as np
from jax import lax

D = 4096
FF = 512
TOP = 2
TOK_DEV = 512
EXPERTS = 16
CAP = 128
TOKENS = 4096
N_EP = 8
N_TP = 4


def draw_tokens(key, part):
    keys = jax.random.split(jax.random.fold_in(key, 11), 2)
    column = jnp.exp(jnp.log(6.0) * jnp.arange(D, dtype=jnp.float32) / (D - 1))
    row_scale = jnp.exp(jax.random.uniform(keys[1], (TOKENS, 1), jnp.float32, 0.0, jnp.log(10.0)))
    base = jax.random.normal(keys[0], (TOKENS, D), jnp.float32)
    base = jnp.clip(base, -5.0, 5.0)
    return (base * column * row_scale / 3.0).astype(jnp.bfloat16)


def shard_levels(own_key, dims, shards, smallest, high):
    loudness = 1.0
    for dim, blocks in shards:
        draws = jax.random.uniform(jax.random.fold_in(jax.random.fold_in(own_key, 6), dim), (blocks,), jnp.float32, smallest / len(shards), high / len(shards))
        loudness = loudness * jnp.repeat(jnp.exp(draws), dims[dim] // blocks).reshape((-1,) + (1,) * (len(dims) - 1 - dim))
    return loudness


def assign_block(key, own, number, rows, amount, top, limit, skew):
    order = jax.random.permutation(key, amount)
    crowded, ordinary = shares(amount, rows * top, limit, skew, True), shares(amount, rows * top, limit, skew, False)
    places = jnp.arange(amount)

    def named(tallies, offset_by):
        used = int((tallies > 0).sum())
        fixed = max(1, used // 4)
        shifted = fixed + (places - fixed + offset_by * (used - fixed)) % max(1, amount - fixed)
        return jnp.zeros((amount,), jnp.int32).at[order[jnp.where(places < fixed, places, shifted)]].set(jnp.asarray(tallies, jnp.int32))

    tallies = jnp.where(number % 4 == 0, named(crowded, number // 4), named(ordinary, number - number // 4 - 1))
    mixed = jax.random.permutation(jax.random.fold_in(own, 3), amount)
    source_of, sink = mixed[0:amount // 2 * 2:2], mixed[1:amount // 2 * 2:2]
    room = jnp.minimum(tallies[source_of] - 1, limit - tallies[sink]) // 2
    room = jnp.where((source_of == order[0]) | (sink == order[0]) | (tallies[sink] == 0), 0, jnp.maximum(room, 0))
    shifted = jax.random.randint(jax.random.fold_in(own, 4), (amount // 2,), 0, 1 << 20) % (room + 1)
    tallies = tallies.at[source_of].add(-shifted).at[sink].add(shifted)
    labels = jnp.searchsorted(jnp.cumsum(tallies), jnp.arange(rows * top), side="right").astype(jnp.int32)
    listing = labels.reshape(top, rows).T
    listing = listing[jax.random.permutation(jax.random.fold_in(own, 1), rows)]
    offset_by = jax.random.randint(jax.random.fold_in(own, 2), (rows, 1), 0, top)
    return jnp.take_along_axis(listing, (jnp.arange(top)[None, :] + offset_by) % top, axis=1)


def shares(amount, total, reach, lean, full):
    loads = [(1 << 20) // math.isqrt(grade ** lean) + 1 for grade in range(1, amount + 1)]
    largest = reach if full else min(reach, max(-(-total // amount), total * loads[0] // sum(loads)))
    least = 1 if total - largest >= amount - 1 else 0
    given, surplus = [largest] + [least] * (amount - 1), total - largest - least * (amount - 1)
    while surplus > 0:
        candidates = [i for i in range(1, amount) if given[i] < largest] or [i for i in range(1, amount) if given[i] < reach]
        pool, left = sum([loads[i] for i in candidates]), surplus
        for i in candidates:
            addition = min(reach - given[i], max(1, left * loads[i] // pool), surplus)
            given[i] = given[i] + addition
            surplus = surplus - addition
    return np.array(given)


def noise(key, shape, scale, bound, pieces=(), kind=jnp.bfloat16):
    result = scale * jax.random.normal(key, shape, jnp.float32)
    if pieces:
        result = result * shard_levels(key, shape, pieces, -0.22, 0.18)
    return jnp.clip(result, -bound, bound).astype(kind)


def setup_inputs(seed: int = 0) -> dict:
    arg_keys = jax.random.split(jax.random.key(seed), 9)
    tokens = draw_tokens(jax.random.fold_in(arg_keys[8], 71), 0)
    routes_keys = jax.random.split(jax.random.fold_in(arg_keys[1], 1), TOKENS // TOK_DEV)
    routes_turns = jax.random.permutation(jax.random.fold_in(arg_keys[1], 3), TOKENS // TOK_DEV)
    routes = jax.vmap(lambda own, number: assign_block(jax.random.fold_in(arg_keys[1], 2), own, number, TOK_DEV, EXPERTS, TOP, CAP, 2))(routes_keys, routes_turns).reshape((TOKENS, TOP))
    route_weights = jnp.clip(0.1 + 0.9 * jax.random.uniform(arg_keys[2], (TOKENS, TOP), jnp.float32) ** shard_levels(arg_keys[2], (TOKENS, TOP), ((0, 8),), -0.2, 0.2), 0.1, 1.0)
    norm_gain = jnp.clip(1.0 + 0.18 * jax.random.normal(arg_keys[3], (D,), jnp.float32), 0.1, 1.9)
    gate_weight = noise(arg_keys[4], (EXPERTS, D, FF), D ** -0.5, 0.09375, ((0, 8), (1, 4)))
    up_weight = noise(arg_keys[5], (EXPERTS, D, FF), D ** -0.5, 0.09375, ((0, 8), (1, 4)))
    down_weight = noise(arg_keys[6], (EXPERTS, FF, D), FF ** -0.5, 0.25, ((0, 8), (2, 4)))
    final_gain = jnp.clip(1.0 + 0.18 * jax.random.normal(arg_keys[7], (D,), jnp.float32), 0.1, 1.9)
    return {"tokens": tokens, "routes": routes, "route_weights": route_weights, "norm_gain": norm_gain, "gate_weight": gate_weight, "up_weight": up_weight, "down_weight": down_weight, "final_gain": final_gain}


EPSILON = 1e-06

def slots_of(chosen):
    experts = jnp.arange(EXPERTS, dtype=jnp.int32)
    onehot = (chosen[:, None] == experts[None, :]).astype(jnp.int32)
    before = jnp.cumsum(onehot, axis=0) - onehot
    return lax.optimization_barrier(jnp.sum(before * onehot, axis=1)).astype(jnp.int32)

def reference(tokens, routes, route_weights, norm_gain, gate_weight, up_weight, down_weight, final_gain):
    values = tokens.astype(jnp.float32)
    scale = lax.rsqrt(lax.optimization_barrier(jnp.mean(values * values, axis=-1, keepdims=True)) + EPSILON)
    normed = (values * scale * norm_gain).astype(jnp.bfloat16)
    count = tokens.shape[0]
    blocks = routes.reshape(N_EP, TOK_DEV * TOP)
    slots = jax.vmap(slots_of)(blocks)
    source = jnp.broadcast_to(jnp.arange(N_EP, dtype=jnp.int32)[:, None], blocks.shape)
    owner = source * TOK_DEV + jnp.arange(TOK_DEV * TOP, dtype=jnp.int32)[None, :] // TOP
    table = jnp.full((EXPERTS, N_EP, CAP), count, jnp.int32).at[blocks, source, slots].set(owner)
    padded = jnp.concatenate([normed, jnp.zeros((1, D), jnp.bfloat16)], axis=0)
    block_width = D // N_TP

    def one_expert(operands):
        index, w_gate, w_up, w_down = operands
        rows = padded[index.reshape(-1)]
        gate = jnp.zeros((rows.shape[0], FF), jnp.float32)
        upper = jnp.zeros((rows.shape[0], FF), jnp.float32)
        for quarter in range(N_TP):
            lower_col = quarter * block_width
            part_rows = rows[:, lower_col:lower_col + block_width]
            gate = gate + jnp.dot(part_rows, w_gate[lower_col:lower_col + block_width], preferred_element_type=jnp.float32).astype(jnp.bfloat16).astype(jnp.float32)
            upper = upper + jnp.dot(part_rows, w_up[lower_col:lower_col + block_width], preferred_element_type=jnp.float32).astype(jnp.bfloat16).astype(jnp.float32)
        hidden = (jax.nn.silu(gate) * upper).astype(jnp.bfloat16)
        return jnp.dot(hidden, w_down, preferred_element_type=jnp.float32).astype(jnp.bfloat16)
    outputs = lax.map(one_expert, (table, gate_weight, up_weight, down_weight))
    returned = outputs.reshape(EXPERTS * N_EP * CAP, D)
    position = (blocks * (N_EP * CAP) + source * CAP + slots).reshape(count, TOP)
    combined = jnp.zeros((count, D), jnp.float32)
    for which in range(TOP):
        combined = combined + route_weights[:, which:which + 1] * returned[position[:, which]].astype(jnp.float32)
    closing = lax.rsqrt(lax.optimization_barrier(jnp.mean(combined * combined, axis=-1, keepdims=True)) + EPSILON)
    return (combined * closing * final_gain).astype(jnp.bfloat16)
```

```python
import functools

import jax
import jax.numpy as jnp
from jax import lax
from jax.experimental import pallas as pl
from jax.experimental.pallas import tpu as pltpu
from jax.sharding import PartitionSpec as P

EPSILON = 1e-06
BF = jnp.bfloat16
F32 = jnp.float32


def dot(a, b):
    return jnp.dot(a, b, preferred_element_type=F32)


def dot_t(a, b):
    return lax.dot_general(a, b, (((0,), (0,)), ((), ())), preferred_element_type=F32)


def kernel(
    n, nt, local, cap,
    x_ref, rank_ref, wt_ref, gate_hbm, up_hbm, down_hbm, out_ref,
    gate_v, up_v, down_v, send_x, recv_x, part, recv_p, hid, out_s, out_r,
    w_sem, xs_sem, xr_sem, ps_sem, pr_sem, hs_sem, hr_sem, os_sem, or_sem,
):
    me = lax.axis_index("ep")
    my_tp = lax.axis_index("tp")
    ff = gate_v.shape[2]
    fq = ff // nt

    loads = [
        pltpu.make_async_copy(src, dst, w_sem.at[i])
        for i, (src, dst) in enumerate(((gate_hbm, gate_v), (up_hbm, up_v), (down_hbm, down_v)))
    ]
    for load in loads:
        load.start()

    barrier = pltpu.get_barrier_semaphore()

    @pl.loop(1, n)
    def _(s):
        pl.semaphore_signal(barrier, inc=1, device_id={"ep": lax.rem(me + s, n), "tp": my_tp})

    for o in range(1, nt):
        pl.semaphore_signal(barrier, inc=1, device_id={"ep": me, "tp": lax.rem(my_tp + o, nt)})

    def onehot(owner, weighted):
        rows = []
        for j in range(local):
            rank = rank_ref[owner * local + j]
            hit = lax.broadcasted_iota(jnp.int32, (cap, rank.shape[1]), 0) == rank
            value = wt_ref[owner * local + j] if weighted else F32(1.0)
            rows.append(jnp.where(hit, value, F32(0.0)))
        return jnp.concatenate(rows, axis=0)

    def pack(owner):
        return dot(onehot(owner, False).astype(BF), x_ref[...]).astype(BF)

    def dest(s):
        return lax.rem(me + s, n)

    def source(s):
        return lax.rem(me - s + n, n)

    def x_copy(s):
        d = dest(s)
        return pltpu.make_async_remote_copy(
            send_x.at[d], recv_x.at[me], xs_sem.at[d], xr_sem.at[me],
            device_id={"ep": d, "tp": my_tp},
        )

    def x_arrival(s):
        b = source(s)
        return pltpu.make_async_remote_copy(
            send_x.at[b], recv_x.at[b], xs_sem.at[b], xr_sem.at[b],
            device_id={"ep": b, "tp": my_tp},
        )

    def p_copy(s, o):
        b = source(s)
        q = lax.rem(my_tp + o, nt)
        return pltpu.make_async_remote_copy(
            part.at[b, q], recv_p.at[b, o - 1], ps_sem.at[b, o - 1], pr_sem.at[b, o - 1],
            device_id={"ep": me, "tp": q},
        )

    def h_copy(s, o):
        b = source(s)
        q = lax.rem(my_tp + o, nt)
        return pltpu.make_async_remote_copy(
            hid.at[b, my_tp], hid.at[b, my_tp], hs_sem.at[b, o - 1], hr_sem.at[b, o - 1],
            device_id={"ep": me, "tp": q},
        )

    def h_arrival(s, o):
        b = source(s)
        q = lax.rem(my_tp - o + nt, nt)
        return pltpu.make_async_remote_copy(
            hid.at[b, q], hid.at[b, q], hs_sem.at[b, o - 1], hr_sem.at[b, o - 1],
            device_id={"ep": me, "tp": q},
        )

    def o_copy(s):
        b = source(s)
        return pltpu.make_async_remote_copy(
            out_s.at[b], out_r.at[me], os_sem.at[b], or_sem.at[me],
            device_id={"ep": b, "tp": my_tp},
        )

    def o_arrival(s):
        d = dest(s)
        return pltpu.make_async_remote_copy(
            out_s.at[d], out_r.at[d], os_sem.at[d], or_sem.at[d],
            device_id={"ep": d, "tp": my_tp},
        )

    def stage_a(s):
        b = source(s)
        for j in range(local):
            rows = recv_x[b, pl.ds(j * cap, cap), :]
            gate = dot(rows, gate_v[j]).astype(BF)
            upper = dot(rows, up_v[j]).astype(BF)
            for q in range(nt):
                part[b, q, pl.ds(j * cap, cap), pl.ds(0, fq)] = gate[:, q * fq:(q + 1) * fq]
                part[b, q, pl.ds(j * cap, cap), pl.ds(fq, fq)] = upper[:, q * fq:(q + 1) * fq]
        for o in range(1, nt):
            p_copy(s, o).start()

    def stage_b(s):
        b = source(s)
        for o in range(1, nt):
            p_copy(s, o).wait_recv()
        total = part[b, my_tp].astype(F32)
        for o in range(1, nt):
            total = total + recv_p[b, o - 1].astype(F32)
        gate, upper = total[:, :fq], total[:, fq:]
        hid[b, my_tp] = (gate / (1.0 + jnp.exp(-gate)) * upper).astype(BF)
        for o in range(1, nt):
            h_copy(s, o).start()

    def stage_c(s, own):
        b = source(s)
        for o in range(1, nt):
            h_arrival(s, o).wait_recv()
        for j in range(local):
            hidden = jnp.concatenate([hid[b, q, pl.ds(j * cap, cap), :] for q in range(nt)], axis=1)
            result = dot(hidden, down_v[j]).astype(BF)
            if own:
                out_r[me, pl.ds(j * cap, cap), :] = result
            else:
                out_s[b, pl.ds(j * cap, cap), :] = result
        if not own:
            o_copy(s).start()

    def combine(s):
        d = dest(s)
        weight = onehot(d, True)
        high = weight.astype(BF)
        low = (weight - high.astype(F32)).astype(BF)
        rows = out_r[d]
        return dot_t(high, rows) + dot_t(low, rows)

    send_x[dest(1)] = pack(dest(1))
    pl.semaphore_wait(barrier, n - 1 + nt - 1)

    @pl.loop(2, n)
    def _(s):
        send_x[dest(s)] = pack(dest(s))
        x_copy(s - 1).start()

    recv_x[me] = pack(me)
    x_copy(n - 1).start()

    for load in loads:
        load.wait()
    stage_a(0)
    x_arrival(1).wait_recv()
    stage_a(1)
    stage_b(0)
    x_arrival(2).wait_recv()
    stage_a(2)
    stage_b(1)
    stage_c(0, True)
    out_ref[...] = combine(0)

    @pl.loop(3, n)
    def _(s):
        x_arrival(s).wait_recv()
        stage_a(s)
        stage_b(s - 1)
        stage_c(s - 2, False)

    stage_b(n - 1)
    stage_c(n - 2, False)
    stage_c(n - 1, False)

    @pl.loop(1, n)
    def _(s):
        o_arrival(s).wait_recv()
        out_ref[...] += combine(s)

    @pl.loop(0, n)
    def _(s):
        for o in range(1, nt):
            p_copy(s, o).wait_send()
            h_copy(s, o).wait_send()

    @pl.loop(1, n)
    def _(s):
        x_copy(s).wait_send()
        o_copy(s).wait_send()


def body(tokens, routes, route_weights, norm_gain, gate_weight, up_weight, down_weight, final_gain):
    n, nt = lax.axis_size("ep"), lax.axis_size("tp")
    local, width, ff = gate_weight.shape
    experts = n * local
    rows = tokens.shape[0]
    full = width * nt
    cap = 4 * rows // experts
    count = local * cap
    values = tokens.astype(F32)
    squares = lax.psum(jnp.sum(values * values, axis=-1), "tp")
    normed = (values * lax.rsqrt(squares / full + EPSILON)[:, None] * norm_gain).astype(BF)
    names = jnp.arange(experts, dtype=jnp.int32)[:, None, None]
    match = routes.T[None, :, :] == names
    hit = jnp.any(match, axis=1)
    weight = jnp.sum(jnp.where(match, route_weights.T[None], 0.0), axis=1)
    steps = jnp.arange(rows, dtype=jnp.int32)
    earlier = (steps[:, None] < steps[None, :]).astype(BF)
    before = dot(hit.astype(BF), earlier).astype(jnp.int32)
    rank = jnp.where(hit, before, -1)

    any_spec = pl.BlockSpec(memory_space=pl.ANY)
    vmem = pl.BlockSpec(memory_space=pltpu.VMEM)
    dma = pltpu.SemaphoreType.DMA
    combined = pl.pallas_call(
        functools.partial(kernel, n, nt, local, cap),
        out_shape=jax.ShapeDtypeStruct((rows, width), F32),
        in_specs=[vmem, vmem, vmem, any_spec, any_spec, any_spec],
        out_specs=vmem,
        scratch_shapes=[
            pltpu.VMEM(gate_weight.shape, BF),
            pltpu.VMEM(up_weight.shape, BF),
            pltpu.VMEM(down_weight.shape, BF),
            pltpu.VMEM((n, count, width), BF),
            pltpu.VMEM((n, count, width), BF),
            pltpu.VMEM((n, nt, count, 2 * ff // nt), BF),
            pltpu.VMEM((n, nt - 1, count, 2 * ff // nt), BF),
            pltpu.VMEM((n, nt, count, ff // nt), BF),
            pltpu.VMEM((n, count, width), BF),
            pltpu.VMEM((n, count, width), BF),
            dma((3,)),
            dma((n,)),
            dma((n,)),
            dma((n, nt - 1)),
            dma((n, nt - 1)),
            dma((n, nt - 1)),
            dma((n, nt - 1)),
            dma((n,)),
            dma((n,)),
        ],
        compiler_params=pltpu.CompilerParams(
            collective_id=0, has_side_effects=True, vmem_limit_bytes=60 * 1024 * 1024
        ),
    )(normed, rank[:, None, :], weight[:, None, :], gate_weight, up_weight, down_weight)
    closing = lax.psum(jnp.sum(combined * combined, axis=-1), "tp")
    return (combined * lax.rsqrt(closing / full + EPSILON)[:, None] * final_gain).astype(BF)


def solution(mesh):
    in_specs = (
        P("ep", "tp"),
        P("ep", None),
        P("ep", None),
        P("tp"),
        P("ep", "tp", None),
        P("ep", "tp", None),
        P("ep", None, "tp"),
        P("tp"),
    )
    return jax.shard_map(body, mesh=mesh, in_specs=in_specs, out_specs=P("ep", "tp"), check_vma=False)
```

```python
import functools

import jax
import jax.numpy as jnp
from jax import lax
from jax.experimental import pallas as pl
from jax.experimental.pallas import tpu as pltpu
from jax.sharding import PartitionSpec as P

EPSILON = 1e-06
BF = jnp.bfloat16
F32 = jnp.float32


def dot(a, b):
    return jnp.dot(a, b, preferred_element_type=F32)


def dot_t(a, b):
    return lax.dot_general(a, b, (((0,), (0,)), ((), ())), preferred_element_type=F32)


def kernel(
    n, nt, local, cap, ring, full,
    x_ref, meta_ref, gain_ref, last_gain_ref, gate_hbm, up_hbm, down_hbm, out_ref,
    gate_v, up_v, down_v, xn, acc, tri, rank_t, wt_t, sq, sq2,
    send_x, recv_x, pk_s, pk_r, far_r, meta_r,
    part, recv_p, hid, out_s, out_r,
    w_sem, xs_sem, xr_sem, ks_sem, kr_sem, fs_sem, fr_sem, ms_sem, mr_sem,
    ps_sem, pr_sem, hs_sem, hr_sem, os_sem, or_sem, qs_sem, qr_sem,
):
    me = lax.axis_index("ep")
    my_tp = lax.axis_index("tp")
    ff = gate_v.shape[2]
    fq = ff // nt
    rows_all = x_ref.shape[0]
    half = n // 2
    chunk = rows_all // 2
    count = local * cap
    split = local // 2

    loads = [
        pltpu.make_async_copy(src, dst, w_sem.at[i])
        for i, (src, dst) in enumerate(((gate_hbm, gate_v), (up_hbm, up_v), (down_hbm, down_v)))
    ]
    for load in loads:
        load.start()

    barrier = pltpu.get_barrier_semaphore()

    @pl.loop(1, n)
    def _(s):
        pl.semaphore_signal(barrier, inc=1, device_id={"ep": lax.rem(me + s, n), "tp": my_tp})

    for o in range(1, nt):
        pl.semaphore_signal(barrier, inc=1, device_id={"ep": me, "tp": lax.rem(my_tp + o, nt)})

    place = jnp.where(me % 2 == 0, me // 2, n - 1 - me // 2)

    def at_place(p):
        p = lax.rem(p + 2 * n, n)
        return jnp.where(p < half, 2 * p, 2 * (n - 1 - p) + 1)

    def shift(s):
        return (1 - 2 * ((s + 1) % 2)) * ((s + 1) // 2)

    def source(s):
        if ring:
            return at_place(place - shift(s))
        return lax.rem(me - s + n, n)

    def sender(s):
        if ring:
            return at_place(place + shift(s))
        return lax.rem(me + s, n)

    def eye():
        shape = (rows_all, rows_all)
        return lax.broadcasted_iota(jnp.int32, shape, 0) == lax.broadcasted_iota(jnp.int32, shape, 1)

    def sq_copy(k, o):
        q = lax.rem(my_tp + o, nt)
        return pltpu.make_async_remote_copy(
            sq.at[k], sq2.at[k, o - 1], qs_sem.at[k, o - 1], qr_sem.at[k, o - 1],
            device_id={"ep": me, "tp": q},
        )

    def start_sum(k, column):
        row = jnp.sum(jnp.where(eye(), column, 0.0), axis=0, keepdims=True)
        sq[k] = jnp.broadcast_to(row, sq.shape[1:])

    def send_sum(k):
        for o in range(1, nt):
            sq_copy(k, o).start()

    def finish_sum(k):
        for o in range(1, nt):
            sq_copy(k, o).wait_recv()
        total = sq[k]
        for o in range(1, nt):
            total = total + sq2[k, o - 1]
        scale = lax.rsqrt(total[0:1] / full + EPSILON)
        return jnp.sum(jnp.where(eye(), scale, 0.0), axis=1, keepdims=True)

    def make_table(slot, meta):
        names = lax.broadcasted_iota(jnp.int32, rank_t.shape[1:], 0).astype(F32)
        first, second = meta[0:1] == names, meta[1:2] == names
        hit = first | second
        before = dot(jnp.where(hit, 1.0, 0.0).astype(BF), tri[...])
        rank_t[slot] = jnp.where(hit, before, -1.0)
        wt_t[slot] = jnp.where(first, meta[2:3], 0.0) + jnp.where(second, meta[3:4], 0.0)

    def onehot(slot, expert, weighted=False):
        rank = rank_t[slot, pl.ds(expert, 1), :]
        hit = lax.broadcasted_iota(jnp.int32, (cap, rows_all), 0).astype(F32) == rank
        return jnp.where(hit, wt_t[slot, pl.ds(expert, 1), :] if weighted else F32(1.0), F32(0.0))

    def pack(slot, experts, block):
        pick = jnp.concatenate([onehot(slot, e) for e in experts], axis=0).astype(BF)
        return dot(pick, block).astype(BF)

    def experts_of(owner):
        return [owner * local + j for j in range(local)]

    def x_copy(s):
        return pltpu.make_async_remote_copy(
            send_x.at[s], recv_x.at[s], xs_sem.at[s], xr_sem.at[s],
            device_id={"ep": sender(s), "tp": my_tp},
        )

    def ahead(i):
        return {"ep": at_place(place + 1 - 2 * i), "tp": my_tp}

    def block_copy(d, i, k):
        piece = pl.ds(k * chunk, chunk)
        src = xn.at[piece] if d == 1 else recv_x.at[2 * d - 4 + i, piece]
        slot = 2 * d - 2 + i
        return pltpu.make_async_remote_copy(
            src, recv_x.at[slot, piece], xs_sem.at[slot, k], xr_sem.at[slot, k], device_id=ahead(i)
        )

    def meta_copy(d, i):
        slot = 2 * d - 2 + i
        return pltpu.make_async_remote_copy(
            meta_ref if d == 1 else meta_r.at[slot - 2], meta_r.at[slot],
            ms_sem.at[slot], mr_sem.at[slot], device_id=ahead(i),
        )

    def pack_copy(i):
        return pltpu.make_async_remote_copy(
            pk_s.at[i], pk_r.at[i], ks_sem.at[i], kr_sem.at[i], device_id=ahead(i)
        )

    def far_copy(i):
        return pltpu.make_async_remote_copy(
            pk_r.at[i, pl.ds(count, split * cap)], far_r.at[i], fs_sem.at[i], fr_sem.at[i],
            device_id=ahead(i),
        )

    def p_copy(s, o):
        q = lax.rem(my_tp + o, nt)
        return pltpu.make_async_remote_copy(
            part.at[s, q], recv_p.at[s, o - 1], ps_sem.at[s, o - 1], pr_sem.at[s, o - 1],
            device_id={"ep": me, "tp": q},
        )

    def h_copy(s, o, back=False):
        mine = lax.rem(my_tp - o + nt, nt) if back else my_tp
        q = lax.rem(my_tp - o + nt, nt) if back else lax.rem(my_tp + o, nt)
        return pltpu.make_async_remote_copy(
            hid.at[s, mine], hid.at[s, mine], hs_sem.at[s, o - 1], hr_sem.at[s, o - 1],
            device_id={"ep": me, "tp": q},
        )

    def o_copy(s):
        return pltpu.make_async_remote_copy(
            out_s.at[s], out_r.at[s], os_sem.at[s], or_sem.at[s],
            device_id={"ep": source(s), "tp": my_tp},
        )

    def stage_a(s, rows_of):
        for j in range(local):
            rows = rows_of(j)
            gate = dot(rows, gate_v[j]).astype(BF)
            upper = dot(rows, up_v[j]).astype(BF)
            for q in range(nt):
                part[s, q, pl.ds(j * cap, cap), pl.ds(0, fq)] = gate[:, q * fq:(q + 1) * fq]
                part[s, q, pl.ds(j * cap, cap), pl.ds(fq, fq)] = upper[:, q * fq:(q + 1) * fq]
        for o in range(1, nt):
            p_copy(s, o).start()

    def stage_b(s):
        for o in range(1, nt):
            p_copy(s, o).wait_recv()
        total = part[s, my_tp].astype(F32)
        for o in range(1, nt):
            total = total + recv_p[s, o - 1].astype(F32)
        gate, upper = total[:, :fq], total[:, fq:]
        hid[s, my_tp] = (gate / (1.0 + jnp.exp(-gate)) * upper).astype(BF)
        for o in range(1, nt):
            h_copy(s, o).start()

    def stage_c(s, own):
        for o in range(1, nt):
            h_copy(s, o, True).wait_recv()
        target = out_r if own else out_s
        for j in range(local):
            hidden = jnp.concatenate([hid[s, q, pl.ds(j * cap, cap), :] for q in range(nt)], axis=1)
            target[s, pl.ds(j * cap, cap), :] = dot(hidden, down_v[j]).astype(BF)
        if not own:
            o_copy(s).start()

    def combine(s):
        weight = jnp.concatenate([onehot(0, e, True) for e in experts_of(sender(s))], axis=0)
        high = weight.astype(BF)
        low = (weight - high.astype(F32)).astype(BF)
        rows = out_r[s]
        return dot_t(high, rows) + dot_t(low, rows)

    values = x_ref[...].astype(F32)
    start_sum(0, jnp.sum(values * values, axis=1, keepdims=True))
    shape = (rows_all, rows_all)
    earlier = lax.broadcasted_iota(jnp.int32, shape, 0) < lax.broadcasted_iota(jnp.int32, shape, 1)
    tri[...] = jnp.where(earlier, 1.0, 0.0).astype(BF)
    pl.semaphore_wait(barrier, n - 1 + nt - 1)
    send_sum(0)
    if ring:
        for i in range(2):
            meta_copy(1, i).start()
    make_table(0, meta_ref[...])
    scale = finish_sum(0)
    xn[...] = (x_ref[...].astype(F32) * scale * gain_ref[...]).astype(BF)

    def own_rows(j):
        return pack(0, [me * local + j], xn[...])

    def stored(ref, slot):
        return lambda j: ref[slot, pl.ds(j * cap, cap), :]

    if ring:
        for k in range(2):
            for i in range(2):
                block_copy(1, i, k).start()
        for load in loads:
            load.wait()
        stage_a(0, own_rows)
        for d in range(1, half + 1):
            if d <= half - 2:
                for k in range(2):
                    for i in range(2):
                        block_copy(d, i, k).wait_recv()
                        if d < half - 2:
                            block_copy(d + 1, i, k).start()
                for i in range(2):
                    slot = 2 * d - 2 + i
                    meta_copy(d, i).wait_recv()
                    if d < half - 2:
                        meta_copy(d + 1, i).start()
                    make_table(1 + slot, meta_r[slot])
                if d == half - 2:
                    for i in range(2):
                        slot = 2 * d - 2 + i
                        step = 1 - 2 * i
                        far = experts_of(at_place(place + 2 * step))
                        wanted = experts_of(at_place(place + step)) + (far[split:] if i else far[:split])
                        pk_s[i] = pack(1 + slot, wanted, recv_x[slot])
                        pack_copy(i).start()
            elif d == half - 1:
                for i in range(2):
                    pack_copy(i).wait_recv()
                    far_copy(i).start()
            else:
                for i in range(2):
                    far_copy(i).wait_recv()
            for i in range(2 if d < half else 1):
                s = 2 * d - 1 + i
                slot = s - 1
                if d <= half - 2:
                    stage_a(s, lambda j, slot=slot: pack(1 + slot, [me * local + j], recv_x[slot]))
                elif d == half - 1:
                    stage_a(s, stored(pk_r, i))
                else:
                    stage_a(s, lambda j: far_r[j // split, pl.ds(j % split * cap, cap), :])
                stage_b(s - 1)
                if s >= 2:
                    stage_c(s - 2, s == 2)
    else:
        send_x[1] = pack(0, experts_of(sender(1)), xn[...])

        @pl.loop(2, n)
        def _(s):
            send_x[s] = pack(0, experts_of(sender(s)), xn[...])
            x_copy(s - 1).start()

        for load in loads:
            load.wait()
        stage_a(0, own_rows)
        x_copy(n - 1).start()
        x_copy(1).wait_recv()
        stage_a(1, stored(recv_x, 1))
        stage_b(0)
        x_copy(2).wait_recv()
        stage_a(2, stored(recv_x, 2))
        stage_b(1)
        stage_c(0, True)

        @pl.loop(3, n)
        def _(s):
            x_copy(s).wait_recv()
            stage_a(s, stored(recv_x, s))
            stage_b(s - 1)
            stage_c(s - 2, False)

    stage_b(n - 1)
    stage_c(n - 2, False)
    acc[...] = combine(0)
    stage_c(n - 1, False)

    @pl.loop(1, n)
    def _(s):
        o_copy(s).wait_recv()
        acc[...] += combine(s)

    summed = acc[...]
    start_sum(1, jnp.sum(summed * summed, axis=1, keepdims=True))

    @pl.loop(0, n)
    def _(s):
        for o in range(1, nt):
            p_copy(s, o).wait_send()
            h_copy(s, o).wait_send()

    send_sum(1)

    @pl.loop(1, n)
    def _(s):
        o_copy(s).wait_send()

    if ring:
        for i in range(2):
            for d in range(1, half - 1):
                meta_copy(d, i).wait_send()
                for k in range(2):
                    block_copy(d, i, k).wait_send()
            pack_copy(i).wait_send()
            far_copy(i).wait_send()
    else:
        @pl.loop(1, n)
        def _(s):
            x_copy(s).wait_send()

    scale = finish_sum(1)
    out_ref[...] = (acc[...] * scale * last_gain_ref[...]).astype(BF)
    for k in range(2):
        for o in range(1, nt):
            sq_copy(k, o).wait_send()


RING_BYTES = 24 * 1024 * 1024


def body(tokens, routes, route_weights, norm_gain, gate_weight, up_weight, down_weight, final_gain):
    n, nt = lax.axis_size("ep"), lax.axis_size("tp")
    local, width, ff = gate_weight.shape
    experts = n * local
    rows = tokens.shape[0]
    full = width * nt
    cap = 4 * rows // experts
    count = local * cap
    blocks = max(n - 4, 0)
    ring = n % 2 == 0 and n >= 6 and local % 2 == 0 and blocks * rows * width * 2 <= RING_BYTES
    meta = jnp.concatenate(
        [routes.T.astype(F32), route_weights.T, jnp.zeros((4, rows), F32)], axis=0
    )
    tables = 1 + blocks if ring else 1
    packed = count + local // 2 * cap

    any_spec = pl.BlockSpec(memory_space=pl.ANY)
    vmem = pl.BlockSpec(memory_space=pltpu.VMEM)
    dma = pltpu.SemaphoreType.DMA

    def only(ring_shape, shape, kind=BF):
        return pltpu.VMEM(ring_shape if ring else shape, kind)

    tiny = (1, 16, 128)
    return pl.pallas_call(
        functools.partial(kernel, n, nt, local, cap, ring, full),
        out_shape=jax.ShapeDtypeStruct((rows, width), BF),
        in_specs=[vmem, vmem, vmem, vmem, any_spec, any_spec, any_spec],
        out_specs=vmem,
        scratch_shapes=[
            pltpu.VMEM(gate_weight.shape, BF),
            pltpu.VMEM(up_weight.shape, BF),
            pltpu.VMEM(down_weight.shape, BF),
            pltpu.VMEM((rows, width), BF),
            pltpu.VMEM((rows, width), F32),
            pltpu.VMEM((rows, rows), BF),
            pltpu.VMEM((tables, experts, rows), F32),
            pltpu.VMEM((tables, experts, rows), F32),
            pltpu.VMEM((2, 8, rows), F32),
            pltpu.VMEM((2, nt - 1, 8, rows), F32),
            only(tiny, (n, count, width)),
            only((blocks, rows, width), (n, count, width)),
            only((2, packed, width), tiny),
            only((2, packed, width), tiny),
            only((2, local // 2 * cap, width), tiny),
            only((blocks, 8, rows), (1, 8, 128), F32),
            pltpu.VMEM((n, nt, count, 2 * ff // nt), BF),
            pltpu.VMEM((n, nt - 1, count, 2 * ff // nt), BF),
            pltpu.VMEM((n, nt, count, ff // nt), BF),
            pltpu.VMEM((n, count, width), BF),
            pltpu.VMEM((n, count, width), BF),
            dma((3,)),
            dma((blocks, 2) if ring else (n,)),
            dma((blocks, 2) if ring else (n,)),
            dma((2,)),
            dma((2,)),
            dma((2,)),
            dma((2,)),
            dma((blocks,) if ring else (1,)),
            dma((blocks,) if ring else (1,)),
            dma((n, nt - 1)),
            dma((n, nt - 1)),
            dma((n, nt - 1)),
            dma((n, nt - 1)),
            dma((n,)),
            dma((n,)),
            dma((2, nt - 1)),
            dma((2, nt - 1)),
        ],
        compiler_params=pltpu.CompilerParams(
            collective_id=0, has_side_effects=True, vmem_limit_bytes=60 * 1024 * 1024
        ),
    )(tokens, meta, norm_gain[None], final_gain[None], gate_weight, up_weight, down_weight)


def solution(mesh):
    in_specs = (
        P("ep", "tp"),
        P("ep", None),
        P("ep", None),
        P("tp"),
        P("ep", "tp", None),
        P("ep", "tp", None),
        P("ep", None, "tp"),
        P("tp"),
    )
    return jax.shard_map(body, mesh=mesh, in_specs=in_specs, out_specs=P("ep", "tp"), check_vma=False)
```

```python
import functools

import jax
import jax.numpy as jnp
from jax import lax
from jax.experimental import pallas as pl
from jax.experimental.pallas import tpu as pltpu
from jax.sharding import PartitionSpec as P

EPSILON = 1e-06
BF = jnp.bfloat16
F32 = jnp.float32


def dot(a, b):
    return jnp.dot(a, b, preferred_element_type=F32)


def dot_t(a, b):
    return lax.dot_general(a, b, (((0,), (0,)), ((), ())), preferred_element_type=F32)


def kernel(
    n, nt, local, cap, ring, full,
    x_ref, meta_ref, gain_ref, last_gain_ref, gate_hbm, up_hbm, down_hbm, out_ref,
    gate_v, up_v, down_v, xn, acc, tri, rank_t, wt_t, sq, sq2,
    send_x, recv_x, pk_s, pk_r, far_r, meta_r, meta_a,
    part, recv_p, hid, out_s, ret, agg_s, agg_r,
    w_sem, xs_sem, xr_sem, ks_sem, kr_sem, fs_sem, fr_sem, ms_sem, mr_sem,
    ps_sem, pr_sem, hs_sem, hr_sem, os_sem, or_sem, qs_sem, qr_sem, as_sem, ar_sem,
):
    me = lax.axis_index("ep")
    my_tp = lax.axis_index("tp")
    ff = gate_v.shape[2]
    fq = ff // nt
    rows_all = x_ref.shape[0]
    half = n // 2
    chunk = rows_all // 2
    count = local * cap
    split = local // 2

    loads = [
        pltpu.make_async_copy(src, dst, w_sem.at[i])
        for i, (src, dst) in enumerate(((gate_hbm, gate_v), (up_hbm, up_v), (down_hbm, down_v)))
    ]
    for load in loads:
        load.start()

    barrier = pltpu.get_barrier_semaphore()

    @pl.loop(1, n)
    def _(s):
        pl.semaphore_signal(barrier, inc=1, device_id={"ep": lax.rem(me + s, n), "tp": my_tp})

    for o in range(1, nt):
        pl.semaphore_signal(barrier, inc=1, device_id={"ep": me, "tp": lax.rem(my_tp + o, nt)})

    def place_of(index):
        return jnp.where(index % 2 == 0, index // 2, n - 1 - index // 2)

    place = place_of(me)
    seat, base = me % half, me // half * half
    opposite = lax.rem(me + half, n)

    def at_place(p):
        p = lax.rem(p + 2 * n, n)
        return jnp.where(p < half, 2 * p, 2 * (n - 1 - p) + 1)

    def shift(s):
        return (1 - 2 * ((s + 1) % 2)) * ((s + 1) // 2)

    def source(s):
        if ring:
            return at_place(place - shift(s))
        return lax.rem(me - s + n, n)

    def opposite_step():
        if not ring:
            return half
        delta = lax.rem(place - place_of(opposite) + n, n)
        return jnp.where(delta <= half, 2 * delta - 1, 2 * (n - delta))

    def sender(s):
        if ring:
            return at_place(place + shift(s))
        return lax.rem(me + s, n)

    def eye():
        shape = (rows_all, rows_all)
        return lax.broadcasted_iota(jnp.int32, shape, 0) == lax.broadcasted_iota(jnp.int32, shape, 1)

    def sq_copy(k, o):
        q = lax.rem(my_tp + o, nt)
        return pltpu.make_async_remote_copy(
            sq.at[k], sq2.at[k, o - 1], qs_sem.at[k, o - 1], qr_sem.at[k, o - 1],
            device_id={"ep": me, "tp": q},
        )

    def start_sum(k, column):
        row = jnp.sum(jnp.where(eye(), column, 0.0), axis=0, keepdims=True)
        sq[k] = jnp.broadcast_to(row, sq.shape[1:])

    def send_sum(k):
        for o in range(1, nt):
            sq_copy(k, o).start()

    def finish_sum(k):
        for o in range(1, nt):
            sq_copy(k, o).wait_recv()
        total = sq[k]
        for o in range(1, nt):
            total = total + sq2[k, o - 1]
        scale = lax.rsqrt(total[0:1] / full + EPSILON)
        return jnp.sum(jnp.where(eye(), scale, 0.0), axis=1, keepdims=True)

    def make_table(slot, meta):
        names = lax.broadcasted_iota(jnp.int32, rank_t.shape[1:], 0).astype(F32)
        first, second = meta[0:1] == names, meta[1:2] == names
        hit = first | second
        before = dot(jnp.where(hit, 1.0, 0.0).astype(BF), tri[...])
        rank_t[slot] = jnp.where(hit, before, -1.0)
        wt_t[slot] = jnp.where(first, meta[2:3], 0.0) + jnp.where(second, meta[3:4], 0.0)

    def onehot(slot, expert, weighted=False):
        rank = rank_t[slot, pl.ds(expert, 1), :]
        hit = lax.broadcasted_iota(jnp.int32, (cap, rows_all), 0).astype(F32) == rank
        return jnp.where(hit, wt_t[slot, pl.ds(expert, 1), :] if weighted else F32(1.0), F32(0.0))

    def pack(slot, experts, block):
        pick = jnp.concatenate([onehot(slot, e) for e in experts], axis=0).astype(BF)
        return dot(pick, block).astype(BF)

    def experts_of(owner):
        return [owner * local + j for j in range(local)]

    def x_copy(s):
        return pltpu.make_async_remote_copy(
            send_x.at[s], recv_x.at[s], xs_sem.at[s], xr_sem.at[s],
            device_id={"ep": sender(s), "tp": my_tp},
        )

    def ahead(i):
        return {"ep": at_place(place + 1 - 2 * i), "tp": my_tp}

    def block_copy(d, i, k):
        piece = pl.ds(k * chunk, chunk)
        src = xn.at[piece] if d == 1 else recv_x.at[2 * d - 4 + i, piece]
        slot = 2 * d - 2 + i
        return pltpu.make_async_remote_copy(
            src, recv_x.at[slot, piece], xs_sem.at[slot, k], xr_sem.at[slot, k], device_id=ahead(i)
        )

    def meta_copy(d, i):
        slot = 2 * d - 2 + i
        return pltpu.make_async_remote_copy(
            meta_ref if d == 1 else meta_r.at[slot - 2], meta_r.at[slot],
            ms_sem.at[slot], mr_sem.at[slot], device_id=ahead(i),
        )

    def pack_copy(i):
        return pltpu.make_async_remote_copy(
            pk_s.at[i], pk_r.at[i], ks_sem.at[i], kr_sem.at[i], device_id=ahead(i)
        )

    def far_copy(i):
        return pltpu.make_async_remote_copy(
            pk_r.at[i, pl.ds(count, split * cap)], far_r.at[i], fs_sem.at[i], fr_sem.at[i],
            device_id=ahead(i),
        )

    def p_copy(s, o):
        q = lax.rem(my_tp + o, nt)
        return pltpu.make_async_remote_copy(
            part.at[s, q], recv_p.at[s, o - 1], ps_sem.at[s, o - 1], pr_sem.at[s, o - 1],
            device_id={"ep": me, "tp": q},
        )

    def h_copy(s, o, back=False):
        mine = lax.rem(my_tp - o + nt, nt) if back else my_tp
        q = lax.rem(my_tp - o + nt, nt) if back else lax.rem(my_tp + o, nt)
        return pltpu.make_async_remote_copy(
            hid.at[s, mine], hid.at[s, mine], hs_sem.at[s, o - 1], hr_sem.at[s, o - 1],
            device_id={"ep": me, "tp": q},
        )

    def o_target(s):
        b = source(s)
        far = jnp.where(b // half == me // half, 0, 1)
        return far, jnp.where(far == 0, b, lax.rem(b + half, n))

    def o_copy(s):
        far, target = o_target(s)
        return pltpu.make_async_remote_copy(
            out_s.at[s], ret.at[far, seat], os_sem.at[s], or_sem.at[far, seat],
            device_id={"ep": target, "tp": my_tp},
        )

    def o_arrival(far, other):
        return pltpu.make_async_remote_copy(
            out_s.at[0], ret.at[far, other], os_sem.at[0], or_sem.at[far, other],
            device_id={"ep": base + other, "tp": my_tp},
        )

    def agg_copy():
        return pltpu.make_async_remote_copy(
            agg_s, agg_r, as_sem.at[0], ar_sem.at[0], device_id={"ep": opposite, "tp": my_tp}
        )

    def agg_meta():
        return pltpu.make_async_remote_copy(
            meta_ref, meta_a, as_sem.at[1], ar_sem.at[1], device_id={"ep": opposite, "tp": my_tp}
        )

    def stage_a(s, rows_of):
        for j in range(local):
            rows = rows_of(j)
            gate = dot(rows, gate_v[j]).astype(BF)
            upper = dot(rows, up_v[j]).astype(BF)
            for q in range(nt):
                part[s, q, pl.ds(j * cap, cap), pl.ds(0, fq)] = gate[:, q * fq:(q + 1) * fq]
                part[s, q, pl.ds(j * cap, cap), pl.ds(fq, fq)] = upper[:, q * fq:(q + 1) * fq]
        for o in range(1, nt):
            p_copy(s, o).start()

    def stage_b(s):
        for o in range(1, nt):
            p_copy(s, o).wait_recv()
        total = part[s, my_tp].astype(F32)
        for o in range(1, nt):
            total = total + recv_p[s, o - 1].astype(F32)
        gate, upper = total[:, :fq], total[:, fq:]
        hid[s, my_tp] = (gate / (1.0 + jnp.exp(-gate)) * upper).astype(BF)
        for o in range(1, nt):
            h_copy(s, o).start()

    def stage_c(s, own):
        for o in range(1, nt):
            h_copy(s, o, True).wait_recv()
        for j in range(local):
            hidden = jnp.concatenate([hid[s, q, pl.ds(j * cap, cap), :] for q in range(nt)], axis=1)
            result = dot(hidden, down_v[j]).astype(BF)
            if own:
                ret[0, seat, pl.ds(j * cap, cap), :] = result
            else:
                out_s[s, pl.ds(j * cap, cap), :] = result
        if not own:
            @pl.when(o_target(s)[1] != me)
            def _():
                o_copy(s).start()

    def combine(slot, owner, rows):
        weight = jnp.concatenate([onehot(slot, e, True) for e in experts_of(owner)], axis=0)
        high = weight.astype(BF)
        low = (weight - high.astype(F32)).astype(BF)
        return dot_t(high, rows) + dot_t(low, rows)

    values = x_ref[...].astype(F32)
    start_sum(0, jnp.sum(values * values, axis=1, keepdims=True))
    shape = (rows_all, rows_all)
    earlier = lax.broadcasted_iota(jnp.int32, shape, 0) < lax.broadcasted_iota(jnp.int32, shape, 1)
    tri[...] = jnp.where(earlier, 1.0, 0.0).astype(BF)
    pl.semaphore_wait(barrier, n - 1 + nt - 1)
    send_sum(0)
    agg_meta().start()
    if ring:
        for i in range(2):
            meta_copy(1, i).start()
    make_table(0, meta_ref[...])
    scale = finish_sum(0)
    xn[...] = (x_ref[...].astype(F32) * scale * gain_ref[...]).astype(BF)

    def own_rows(j):
        return pack(0, [me * local + j], xn[...])

    def stored(ref, slot):
        return lambda j: ref[slot, pl.ds(j * cap, cap), :]

    if ring:
        for k in range(2):
            for i in range(2):
                block_copy(1, i, k).start()
        for load in loads:
            load.wait()
        stage_a(0, own_rows)
        for d in range(1, half + 1):
            if d <= half - 2:
                for k in range(2):
                    for i in range(2):
                        block_copy(d, i, k).wait_recv()
                        if d < half - 2:
                            block_copy(d + 1, i, k).start()
                for i in range(2):
                    slot = 2 * d - 2 + i
                    meta_copy(d, i).wait_recv()
                    if d < half - 2:
                        meta_copy(d + 1, i).start()
                    make_table(1 + slot, meta_r[slot])
                if d == half - 2:
                    for i in range(2):
                        slot = 2 * d - 2 + i
                        step = 1 - 2 * i
                        far = experts_of(at_place(place + 2 * step))
                        wanted = experts_of(at_place(place + step)) + (far[split:] if i else far[:split])
                        pk_s[i] = pack(1 + slot, wanted, recv_x[slot])
                        pack_copy(i).start()
            elif d == half - 1:
                for i in range(2):
                    pack_copy(i).wait_recv()
                    far_copy(i).start()
            else:
                for i in range(2):
                    far_copy(i).wait_recv()
            for i in range(2 if d < half else 1):
                s = 2 * d - 1 + i
                slot = s - 1
                if d <= half - 2:
                    stage_a(s, lambda j, slot=slot: pack(1 + slot, [me * local + j], recv_x[slot]))
                elif d == half - 1:
                    stage_a(s, stored(pk_r, i))
                else:
                    stage_a(s, lambda j: far_r[j // split, pl.ds(j % split * cap, cap), :])
                stage_b(s - 1)
                if s >= 2:
                    stage_c(s - 2, s == 2)
    else:
        send_x[1] = pack(0, experts_of(sender(1)), xn[...])

        @pl.loop(2, n)
        def _(s):
            send_x[s] = pack(0, experts_of(sender(s)), xn[...])
            x_copy(s - 1).start()

        for load in loads:
            load.wait()
        stage_a(0, own_rows)
        x_copy(n - 1).start()
        x_copy(1).wait_recv()
        stage_a(1, stored(recv_x, 1))
        stage_b(0)
        x_copy(2).wait_recv()
        stage_a(2, stored(recv_x, 2))
        stage_b(1)
        stage_c(0, True)

        @pl.loop(3, n)
        def _(s):
            x_copy(s).wait_recv()
            stage_a(s, stored(recv_x, s))
            stage_b(s - 1)
            stage_c(s - 2, False)

    stage_b(n - 1)
    stage_c(n - 2, False)
    stage_c(n - 1, False)
    agg_meta().wait_recv()
    last = rank_t.shape[0] - 1
    make_table(last, meta_a[...])
    acc[...] = combine(last, me, out_s[opposite_step()])

    @pl.loop(1, half)
    def _(k):
        other = lax.rem(seat + k, half)
        o_arrival(1, other).wait_recv()
        acc[...] += combine(last, base + other, ret[1, other])

    agg_s[...] = acc[...].astype(BF)
    acc[...] = combine(0, me, ret[0, seat])
    agg_copy().start()

    @pl.loop(1, half)
    def _(k):
        other = lax.rem(seat + k, half)
        o_arrival(0, other).wait_recv()
        acc[...] += combine(0, base + other, ret[0, other])

    agg_copy().wait_recv()
    acc[...] += agg_r[...].astype(F32)
    summed = acc[...]
    start_sum(1, jnp.sum(summed * summed, axis=1, keepdims=True))

    @pl.loop(0, n)
    def _(s):
        for o in range(1, nt):
            p_copy(s, o).wait_send()
            h_copy(s, o).wait_send()

    send_sum(1)

    @pl.loop(1, n)
    def _(s):
        @pl.when(o_target(s)[1] != me)
        def _():
            o_copy(s).wait_send()

    agg_copy().wait_send()
    agg_meta().wait_send()

    if ring:
        for i in range(2):
            for d in range(1, half - 1):
                meta_copy(d, i).wait_send()
                for k in range(2):
                    block_copy(d, i, k).wait_send()
            pack_copy(i).wait_send()
            far_copy(i).wait_send()
    else:
        @pl.loop(1, n)
        def _(s):
            x_copy(s).wait_send()

    scale = finish_sum(1)
    out_ref[...] = (acc[...] * scale * last_gain_ref[...]).astype(BF)
    for k in range(2):
        for o in range(1, nt):
            sq_copy(k, o).wait_send()


RING_BYTES = 24 * 1024 * 1024


def body(tokens, routes, route_weights, norm_gain, gate_weight, up_weight, down_weight, final_gain):
    n, nt = lax.axis_size("ep"), lax.axis_size("tp")
    local, width, ff = gate_weight.shape
    experts = n * local
    rows = tokens.shape[0]
    full = width * nt
    cap = 4 * rows // experts
    count = local * cap
    blocks = max(n - 4, 0)
    ring = n % 2 == 0 and n >= 6 and local % 2 == 0 and blocks * rows * width * 2 <= RING_BYTES
    meta = jnp.concatenate(
        [routes.T.astype(F32), route_weights.T, jnp.zeros((4, rows), F32)], axis=0
    )
    tables = 2 + blocks if ring else 2
    packed = count + local // 2 * cap

    any_spec = pl.BlockSpec(memory_space=pl.ANY)
    vmem = pl.BlockSpec(memory_space=pltpu.VMEM)
    dma = pltpu.SemaphoreType.DMA

    def only(ring_shape, shape, kind=BF):
        return pltpu.VMEM(ring_shape if ring else shape, kind)

    tiny = (1, 16, 128)
    return pl.pallas_call(
        functools.partial(kernel, n, nt, local, cap, ring, full),
        out_shape=jax.ShapeDtypeStruct((rows, width), BF),
        in_specs=[vmem, vmem, vmem, vmem, any_spec, any_spec, any_spec],
        out_specs=vmem,
        scratch_shapes=[
            pltpu.VMEM(gate_weight.shape, BF),
            pltpu.VMEM(up_weight.shape, BF),
            pltpu.VMEM(down_weight.shape, BF),
            pltpu.VMEM((rows, width), BF),
            pltpu.VMEM((rows, width), F32),
            pltpu.VMEM((rows, rows), BF),
            pltpu.VMEM((tables, experts, rows), F32),
            pltpu.VMEM((tables, experts, rows), F32),
            pltpu.VMEM((2, 8, rows), F32),
            pltpu.VMEM((2, nt - 1, 8, rows), F32),
            only(tiny, (n, count, width)),
            only((blocks, rows, width), (n, count, width)),
            only((2, packed, width), tiny),
            only((2, packed, width), tiny),
            only((2, local // 2 * cap, width), tiny),
            only((blocks, 8, rows), (1, 8, 128), F32),
            pltpu.VMEM((8, rows), F32),
            pltpu.VMEM((n, nt, count, 2 * ff // nt), BF),
            pltpu.VMEM((n, nt - 1, count, 2 * ff // nt), BF),
            pltpu.VMEM((n, nt, count, ff // nt), BF),
            pltpu.VMEM((n, count, width), BF),
            pltpu.VMEM((2, n // 2, count, width), BF),
            pltpu.VMEM((rows, width), BF),
            pltpu.VMEM((rows, width), BF),
            dma((3,)),
            dma((blocks, 2) if ring else (n,)),
            dma((blocks, 2) if ring else (n,)),
            dma((2,)),
            dma((2,)),
            dma((2,)),
            dma((2,)),
            dma((blocks,) if ring else (1,)),
            dma((blocks,) if ring else (1,)),
            dma((n, nt - 1)),
            dma((n, nt - 1)),
            dma((n, nt - 1)),
            dma((n, nt - 1)),
            dma((n,)),
            dma((2, n // 2)),
            dma((2, nt - 1)),
            dma((2, nt - 1)),
            dma((2,)),
            dma((2,)),
        ],
        compiler_params=pltpu.CompilerParams(
            collective_id=0, has_side_effects=True, vmem_limit_bytes=60 * 1024 * 1024
        ),
    )(tokens, meta, norm_gain[None], final_gain[None], gate_weight, up_weight, down_weight)


def solution(mesh):
    in_specs = (
        P("ep", "tp"),
        P("ep", None),
        P("ep", None),
        P("tp"),
        P("ep", "tp", None),
        P("ep", "tp", None),
        P("ep", None, "tp"),
        P("tp"),
    )
    return jax.shard_map(body, mesh=mesh, in_specs=in_specs, out_specs=P("ep", "tp"), check_vma=False)
```
